32 devices in a mesh: ep: 8 (over z, x), tp: 4 (over y, core).
Axes of the slice: x: 2, y: 2, z: 4, core: 2. Of those that a mesh axis runs over, the one named last changes fastest.
Arguments:
- tokens: bfloat16 [256, 4096], P('ep'), may hold values from -6 to 6
- norm_gain: float32 [4096], replicated, may hold values from 0.1 to 1.9
- routes: int32 [256, 4], P('ep'), may hold values from 0 to 15, as said below
- group_prob: float32 [256], P('ep'), may hold values from 0.25 to 1
- expert_scores: float32 [256, 4], P('ep'), may hold values from -4 to 4
- gate_weight: bfloat16 [16, 1024, 4096], P('ep', 'tp'), may hold values from -0.09375 to 0.09375
- up_weight: bfloat16 [16, 1024, 4096], P('ep', 'tp'), may hold values from -0.09375 to 0.09375
- down_weight: bfloat16 [16, 1024, 4096], P('ep', 'tp'), may hold values from -0.1875 to 0.1875
Outputs:
- moe_out: bfloat16 [256, 4096], P('ep', 'tp')
The draws below stay inside these ranges and needn't reach their ends.
Inputs may be any that keep to these rules, and one draw needn't show every extreme that they name: `routes`: the 4 entries of a row are distinct and lie in one group, ids g * 8 to g * 8 + 7. In each aligned block of 32 rows (the tokens of one ep index) at most 32 rows choose any one group, so at most 32 rows name an expert of any one ep index; in every block some ep index is named by exactly 32 rows.
All inputs are finite; a program needn't handle non-finite values.
Results may differ from the reference program's by a relative error of at most 0.018.
Values may be sent and summed in bfloat16 or wider, within the bound.
A program may use at most 64 MiB of HBM per device.

```python
import math
import jax
import jax.numpy as jnp
from jax import lax

D = 4096
FF = 1024
EXP_DEV = 2
EXP_GROUP = 8
TOPK = 4
TOK_EP = 32
TOKENS = 256
EXPERTS = 16
GROUPS = 2
GCAP = 32
N_EP = 8
N_TP = 4


def route_block(block_key, relabel):
    keys = jax.random.split(block_key, 7)
    hot_group = jnp.minimum(jax.random.randint(keys[0], (), 0, GROUPS), jax.random.randint(keys[1], (), 0, GROUPS))
    slot_group = jnp.arange(GROUPS * GCAP, dtype=jnp.int32) // GCAP
    ordering = jax.random.permutation(keys[2], GROUPS * GCAP).astype(jnp.int32)
    priority = ordering - (slot_group == hot_group).astype(jnp.int32) * (GROUPS * GCAP)
    picked = jnp.argsort(priority)[:TOK_EP]
    chosen_group = slot_group[picked]
    chosen_group = chosen_group[jax.random.permutation(keys[3], TOK_EP)]
    hot_device = jax.random.randint(keys[4], (), 0, EXP_GROUP // EXP_DEV)
    inner_keys = jax.random.split(keys[5], TOK_EP)
    inner_rank = jax.vmap(lambda one_key: jax.random.permutation(one_key, EXP_GROUP))(inner_keys).astype(jnp.int32)
    inner_ids = jnp.arange(EXP_GROUP, dtype=jnp.int32)
    forced = (chosen_group == hot_group)[:, None] & (inner_ids // EXP_DEV == hot_device)[None, :]
    inner_priority = inner_rank - forced.astype(jnp.int32) * EXP_GROUP
    inner_pick = jnp.argsort(inner_priority, axis=1)[:, :TOPK].astype(jnp.int32)
    final_group = relabel[chosen_group]
    return (final_group[:, None] * EXP_GROUP + inner_pick).astype(jnp.int32)


def draw_routes(key, part):
    label_key = jax.random.fold_in(key, 11)
    relabel = jax.random.permutation(label_key, GROUPS).astype(jnp.int32)
    block_keys = jax.random.split(jax.random.fold_in(key, 23), TOKENS // TOK_EP)
    routed = jax.vmap(lambda one_key: route_block(one_key, relabel))(block_keys)
    return routed.reshape(TOKENS, TOPK).astype(jnp.int32)


def block_levels(rng, dims, cuts, smallest, largest):
    factor_of, own = 1.0, jax.random.fold_in(rng, 6)
    for position, shards_of in cuts:
        heights = jnp.exp(jax.random.uniform(jax.random.fold_in(own, position), (shards_of,), jnp.float32, smallest / len(cuts), largest / len(cuts)))
        factor_of = factor_of * jnp.repeat(heights, dims[position] // shards_of).reshape([-1 if axis == position else 1 for axis in range(len(dims))])
    return factor_of


def noise(own_key, shape, deviation, most, pieces=(), kind=jnp.bfloat16):
    factor_of = block_levels(own_key, shape, pieces, -0.22, 0.18) if pieces else 1.0
    values = jax.random.normal(own_key, shape, jnp.float32) * deviation * factor_of
    return jnp.minimum(jnp.maximum(values, -most), most).astype(kind)


def setup_inputs(seed: int = 0) -> dict:
    streams_of = jax.random.split(jax.random.key(seed), 9)
    tokens = noise(streams_of[0], (TOKENS, D), 1.0, 6.0, ((0, 8),))
    norm_gain = jnp.clip(1.0 + 0.18 * jax.random.normal(streams_of[1], (D,), jnp.float32), 0.1, 1.9)
    routes = draw_routes(jax.random.fold_in(streams_of[8], 71), 0)
    group_prob = jnp.clip(jnp.exp(math.log(1.0) - 1.3862944 * jax.random.uniform(streams_of[3], (TOKENS,), jnp.float32) ** block_levels(streams_of[3], (TOKENS,), ((0, 8),), -0.2, 0.2)), 0.25, 1.0)
    expert_scores = noise(streams_of[4], (TOKENS, TOPK), 1.0, 4.0, ((0, 8),), jnp.float32)
    gate_weight = noise(streams_of[5], (EXPERTS, FF, D), D ** -0.5, 0.09375, ((0, 8), (1, 4)))
    up_weight = noise(streams_of[6], (EXPERTS, FF, D), D ** -0.5, 0.09375, ((0, 8), (1, 4)))
    down_weight = noise(streams_of[7], (EXPERTS, FF, D), FF ** -0.5, 0.1875, ((0, 8), (1, 4)))
    return {"tokens": tokens, "norm_gain": norm_gain, "routes": routes, "group_prob": group_prob, "expert_scores": expert_scores, "gate_weight": gate_weight, "up_weight": up_weight, "down_weight": down_weight}


EPS = 1e-06

def device_work(args):
    rows, weights, gate_w, up_w, down_w = args
    rows_f = rows.astype(jnp.float32)
    gate_act = jnp.einsum('rd,jfd->rjf', rows_f, gate_w.astype(jnp.float32))
    up_act = jnp.einsum('rd,jfd->rjf', rows_f, up_w.astype(jnp.float32))
    hidden = (jax.nn.silu(gate_act) * up_act * weights.astype(jnp.float32)[:, :, None]).astype(jnp.bfloat16)
    block_width = FF // N_TP
    count = rows.shape[0]
    partial_value = jnp.einsum('rjtf,jtfd->rtd', hidden.reshape(count, EXP_DEV, N_TP, block_width).astype(jnp.float32), down_w.reshape(EXP_DEV, N_TP, block_width, D).astype(jnp.float32))
    rounded = lax.optimization_barrier(partial_value.astype(jnp.bfloat16))
    return lax.optimization_barrier(jnp.sum(rounded.astype(jnp.float32), axis=1)).astype(jnp.bfloat16)

def place_block(args):
    slots, rows, weights = args
    flat_slots = slots.reshape(-1).astype(jnp.int32)
    spread_rows = jnp.broadcast_to(rows[:, None, :], (TOK_EP, N_EP, D)).reshape(TOK_EP * N_EP, D)
    row_buf = jnp.zeros((N_EP * GCAP, D), jnp.bfloat16).at[flat_slots].set(spread_rows, mode='drop')
    weight_buf = jnp.zeros((N_EP * GCAP, EXP_DEV), jnp.bfloat16).at[flat_slots].set(weights.reshape(TOK_EP * N_EP, EXP_DEV).astype(jnp.bfloat16), mode='drop')
    return (row_buf, weight_buf)

def take_rows(rows, slot_ids):
    return rows[slot_ids]

def reference(tokens, norm_gain, routes, group_prob, expert_scores, gate_weight, up_weight, down_weight):
    as_float = tokens.astype(jnp.float32)
    normed = (as_float * lax.rsqrt(lax.optimization_barrier(jnp.mean(as_float * as_float, axis=-1, keepdims=True)) + EPS) * norm_gain).astype(jnp.bfloat16)
    mixing = jax.nn.softmax(expert_scores.astype(jnp.float32), axis=-1) * group_prob[:, None]
    mixing_half = mixing.astype(jnp.bfloat16)
    blocks = TOKENS // TOK_EP
    routes = routes.astype(jnp.int32)
    dev_of = (routes // EXP_DEV).astype(jnp.int32)
    dev_ids = jnp.arange(N_EP, dtype=jnp.int32)
    touch = jnp.any(dev_of[:, :, None] == dev_ids[None, None, :], axis=1)
    rank = (jnp.cumsum(touch.astype(jnp.int32).reshape(blocks, TOK_EP, N_EP), axis=1) - 1).reshape(TOKENS, N_EP)
    slot_td = jnp.where(touch, dev_ids[None, :] * GCAP + rank, N_EP * GCAP).astype(jnp.int32)
    onehot = (routes[:, :, None] == jnp.arange(EXPERTS, dtype=jnp.int32)[None, None, :]).astype(jnp.float32)
    weights = jnp.einsum('tke,tk->te', onehot, mixing_half.astype(jnp.float32), precision=lax.Precision.HIGHEST).reshape(TOKENS, N_EP, EXP_DEV)
    row_bufs, weight_bufs = lax.map(place_block, (slot_td.reshape(blocks, TOK_EP, N_EP), normed.reshape(blocks, TOK_EP, D), weights.reshape(blocks, TOK_EP, N_EP, EXP_DEV)))
    per_dev_rows = row_bufs.reshape(blocks, N_EP, GCAP, D).transpose(1, 0, 2, 3).reshape(N_EP, blocks * GCAP, D)
    per_dev_w = weight_bufs.reshape(blocks, N_EP, GCAP, EXP_DEV).transpose(1, 0, 2, 3).reshape(N_EP, blocks * GCAP, EXP_DEV)
    outputs = lax.map(device_work, (per_dev_rows, per_dev_w, gate_weight.reshape(N_EP, EXP_DEV, FF, D), up_weight.reshape(N_EP, EXP_DEV, FF, D), down_weight.reshape(N_EP, EXP_DEV, FF, D)))
    outputs = outputs.reshape(N_EP, blocks, GCAP, D).transpose(1, 0, 2, 3).reshape(blocks, N_EP * GCAP, D)
    slot_tk = jnp.take_along_axis(slot_td, dev_of, axis=1).astype(jnp.int32)
    order = jnp.arange(TOPK, dtype=jnp.int32)
    earlier = (dev_of[:, :, None] == dev_of[:, None, :]) & (order[None, None, :] < order[None, :, None])
    first = jnp.logical_not(jnp.any(earlier, axis=2)).astype(jnp.float32)
    picked = jax.vmap(take_rows)(outputs, slot_tk.reshape(blocks, TOK_EP * TOPK))
    picked = picked.reshape(TOKENS, TOPK, D).astype(jnp.float32)
    return lax.optimization_barrier(jnp.sum(first[:, :, None] * picked, axis=1)).astype(jnp.bfloat16)
```

```python
import functools

import jax
import jax.numpy as jnp
from jax import lax
from jax.experimental import pallas as pl
from jax.experimental.pallas import tpu as pltpu
from jax.sharding import PartitionSpec as P

EXP_GROUP = 8


EPS = 1e-06


def body(tokens, norm_gain, routes, group_prob, expert_scores, gate_weight, up_weight, down_weight):
    ep_count = lax.axis_size("ep")
    tp_count = lax.axis_size("tp")
    token_count, model_width = tokens.shape
    expert_local = gate_weight.shape[0]
    expert_total = expert_local * ep_count
    group_total = expert_total // EXP_GROUP
    cap_slots = min(token_count, 2 * ((token_count + group_total - 1) // group_total))
    slot_total = ep_count * cap_slots
    as_float = tokens.astype(jnp.float32)
    normed = (
        as_float
        * lax.rsqrt(jnp.mean(as_float * as_float, axis=-1, keepdims=True) + EPS)
        * norm_gain
    ).astype(jnp.bfloat16)
    mixing = jax.nn.softmax(expert_scores, axis=-1) * group_prob[:, None]
    mixing_half = mixing.astype(jnp.bfloat16)
    dev_of = routes // expert_local
    dev_ids = jnp.arange(ep_count, dtype=jnp.int32)
    touch = jnp.any(dev_of[:, :, None] == dev_ids[None, None, :], axis=1)
    rank = jnp.cumsum(touch.astype(jnp.int32), axis=0) - 1
    slot_td = jnp.where(touch, dev_ids[None, :] * cap_slots + rank, -1)
    slot_range = jnp.arange(slot_total, dtype=jnp.int32)
    matches = jnp.any(slot_td[None, :, :] == slot_range[:, None, None], axis=2)
    onehot = (
        routes[:, :, None] == jnp.arange(expert_total, dtype=jnp.int32)[None, None, :]
    ).astype(jnp.float32)
    weights = jnp.einsum(
        "tke,tk->te", onehot, mixing_half.astype(jnp.float32), precision=lax.Precision.HIGHEST
    ).reshape(token_count, ep_count, expert_local)
    out_weights = jnp.einsum(
        "dct,tdj->dcj",
        matches.reshape(ep_count, cap_slots, token_count).astype(jnp.float32),
        weights,
        precision=lax.Precision.HIGHEST,
    ).astype(jnp.bfloat16)
    share = model_width // tp_count
    payload = lax.dynamic_slice_in_dim(normed, lax.axis_index("tp") * share, share, 1)
    outgoing = jnp.dot(
        matches.astype(jnp.bfloat16), payload, preferred_element_type=jnp.float32
    ).astype(jnp.bfloat16)
    outgoing = outgoing.reshape(ep_count, cap_slots, payload.shape[1])
    rows = lax.all_to_all(outgoing, "ep", split_axis=0, concat_axis=0, tiled=True)
    row_weights = lax.all_to_all(out_weights, "ep", split_axis=0, concat_axis=0, tiled=True)
    rows = lax.all_gather(rows, "tp", axis=2, tiled=True)
    gate_act = jnp.einsum("scd,jfd->scjf", rows, gate_weight, preferred_element_type=jnp.float32)
    up_act = jnp.einsum("scd,jfd->scjf", rows, up_weight, preferred_element_type=jnp.float32)
    hidden = (
        jax.nn.silu(gate_act) * up_act * row_weights.astype(jnp.float32)[:, :, :, None]
    ).astype(jnp.bfloat16)
    partial_value = jnp.einsum(
        "scjf,jfd->scd", hidden, down_weight, preferred_element_type=jnp.float32
    ).astype(jnp.bfloat16)
    summed = lax.psum_scatter(partial_value, "tp", scatter_dimension=2, tiled=True).astype(
        jnp.float32
    )
    returned = lax.all_to_all(
        summed.astype(jnp.bfloat16), "ep", split_axis=0, concat_axis=0, tiled=True
    )
    gathered_rows = returned.reshape(slot_total, returned.shape[2]).astype(jnp.float32)
    result = jnp.dot(matches.T.astype(jnp.float32), gathered_rows, precision=lax.Precision.HIGHEST)
    return result.astype(jnp.bfloat16)


GROUP_Z = 2
LANES = 128
GATHER_NUM, GATHER_DEN = 5, 8
MESH = pl.DeviceIdType.MESH


def kernel(
    nz, tokens, gain, routes, prob, scores, gate_hbm, up_hbm, down_hbm, out,
    tok, gain_v, routes_v, prob_v, scores_v, wg, wu, wd, xbuf, wbuf, acc, pcs, pcr,
    y1s, y1r, x1s, x1r, y2s, y2r, x2s, x2r, zs, zr, own,
    loc, azs, azr, wzs, wzr, axs, axr, wxs, wxr, ays, ayr, acs, acr,
    rcs, rcr, ry1s, ry1r, rx1s, rx1r, ry2s, ry2r, rx2s, rx2r, rzs, rzr,
):
    ep, tp = lax.axis_index("ep"), lax.axis_index("tp")
    z, x = ep // 2, ep % 2
    y, c = tp // 2, tp % 2
    rows, width = tokens.shape
    el, hid, _ = gate_hbm.shape
    ng = nz // GROUP_Z
    grows = 2 * GROUP_Z * rows
    half = width // 2
    quarter = width // 4
    part = quarter // 2
    gcols = half * GATHER_NUM // GATHER_DEN
    ycols = half - gcols

    def dev(z_, x_, y_, c_):
        return (z_ * 2 + x_, y_ * 2 + c_)

    xdev, ydev, cdev = dev(z, 1 - x, y, c), dev(z, x, 1 - y, c), dev(z, x, y, 1 - c)
    zof = [lax.rem(z + d, nz) for d in range(nz)]

    def rc(src, dst, ss, rs, to):
        return pltpu.make_async_remote_copy(
            src_ref=src, dst_ref=dst, send_sem=ss, recv_sem=rs, device_id=to, device_id_type=MESH
        )

    pairs = [
        (tokens, tok), (gain, gain_v), (routes, routes_v), (prob, prob_v), (scores, scores_v),
        (gate_hbm, wg), (up_hbm, wu), (down_hbm, wd),
    ]
    local = [pltpu.make_async_copy(s, d, loc.at[i]) for i, (s, d) in enumerate(pairs)]
    for cp in local:
        cp.start()
    barrier = pltpu.get_barrier_semaphore()
    friends = [xdev, ydev, cdev] + [dev(zz, x, y, c) for zz in zof[1:]]
    for to in friends:
        pl.semaphore_signal(barrier, inc=1, device_id=to, device_id_type=MESH)

    def slot(z_, x_):
        return ((z_ // 2) * 2 + x_) * 2 + z_ % 2

    def rowsof(s):
        return pl.ds(pl.multiple_of(s * rows, rows), rows)

    for cp in local[:5]:
        cp.wait()
    mine = slot(z, x)
    step = 16
    wide = 4 * LANES
    for r in range(0, rows, step):
        total = jnp.zeros((step, wide), jnp.float32)
        for k in range(0, width, wide):
            v = tok[r : r + step, k : k + wide].astype(jnp.float32)
            total += v * v
        scale = lax.rsqrt(jnp.sum(total, axis=1, keepdims=True) / width + EPS)
        at = pl.ds(pl.multiple_of(mine * rows + r, step), step)
        for k in range(0, width, wide):
            v = tok[r : r + step, k : k + wide].astype(jnp.float32)
            xbuf[at, k : k + wide] = (v * scale * gain_v[:, k : k + wide]).astype(jnp.bfloat16)
    diag = lax.broadcasted_iota(jnp.int32, (rows, rows), 0) == lax.broadcasted_iota(
        jnp.int32, (rows, rows), 1
    )
    pcol = jnp.sum(jnp.where(diag, jnp.broadcast_to(prob_v[...], (rows, rows)), 0.0), axis=1, keepdims=True)
    s = scores_v[...]
    e = jnp.exp(s - jnp.max(s, axis=1, keepdims=True))
    mix = (e / jnp.sum(e, axis=1, keepdims=True) * pcol).astype(jnp.bfloat16).astype(jnp.float32)
    lane = lax.broadcasted_iota(jnp.int32, (rows, wbuf.shape[1]), 1)
    wm = jnp.zeros((rows, wbuf.shape[1]), jnp.float32)
    rt = routes_v[...]
    for k in range(rt.shape[1]):
        wm += jnp.where(rt[:, k : k + 1] == lane, mix[:, k : k + 1], 0.0)
    wbuf[rowsof(mine), :] = wm.astype(jnp.bfloat16)

    pl.semaphore_wait(barrier, len(friends))

    gc = pl.ds(pl.multiple_of(c * half + y * ycols, LANES), gcols)
    ysend = pl.ds(pl.multiple_of(c * half + y * gcols, LANES), ycols)
    yrecv = pl.ds(pl.multiple_of(c * half + (1 - y) * gcols, LANES), ycols)
    csend = pl.ds(pl.multiple_of(c * half, LANES), half)
    crecv = pl.ds(pl.multiple_of((1 - c) * half, LANES), half)

    sends = []

    def go(cp):
        cp.start()
        sends.append(cp)

    def x_out(zz):
        b = rowsof(slot(zz, x))
        go(rc(xbuf.at[b, gc], xbuf.at[b, gc], axs.at[zz], axr.at[zz], xdev))
        go(rc(wbuf.at[b], wbuf.at[b], wxs.at[zz], wxr.at[zz], xdev))

    def y_out(s_):
        b = rowsof(s_)
        go(rc(xbuf.at[b, ysend], xbuf.at[b, ysend], ays.at[s_], ayr.at[s_], ydev))

    b = rowsof(mine)
    order = [d for d in range(1, nz)]
    x_out(z)

    zp = z // 2
    inner = zp * 2 + 1 - z % 2
    outer = [(lax.rem(zp + g, ng) * 2 + low, g) for g in range(1, ng) for low in range(2)]
    for zz in [inner] + [o for o, _ in outer]:
        go(rc(xbuf.at[b, gc], xbuf.at[b, gc], azs.at[zz], azr.at[z], dev(zz, x, y, c)))
        go(rc(wbuf.at[b], wbuf.at[b], wzs.at[zz], wzr.at[z], dev(zz, x, y, c)))

    def z_in(zz):
        r_ = rowsof(slot(zz, x))
        to = dev(zz, x, y, c)
        rc(xbuf.at[r_, gc], xbuf.at[r_, gc], azs.at[zz], azr.at[zz], to).wait_recv()
        rc(wbuf.at[r_], wbuf.at[r_], wzs.at[zz], wzr.at[zz], to).wait_recv()
        x_out(zz)
        y_out(slot(zz, x))

    def x_in(zz):
        r_ = rowsof(slot(zz, 1 - x))
        rc(xbuf.at[r_, gc], xbuf.at[r_, gc], axs.at[zz], axr.at[zz], xdev).wait_recv()
        rc(wbuf.at[r_], wbuf.at[r_], wxs.at[zz], wxr.at[zz], xdev).wait_recv()
        y_out(slot(zz, 1 - x))

    def y_in(s_):
        r_ = rowsof(s_)
        rc(xbuf.at[r_, yrecv], xbuf.at[r_, yrecv], ays.at[s_], ayr.at[s_], ydev).wait_recv()
        go(rc(xbuf.at[r_, csend], xbuf.at[r_, csend], acs.at[s_], acr.at[s_], cdev))

    def c_in(s_):
        r_ = rowsof(s_)
        rc(xbuf.at[r_, crecv], xbuf.at[r_, crecv], acs.at[s_], acr.at[s_], cdev).wait_recv()

    near = [slot(inner, x), slot(z, 1 - x), slot(inner, 1 - x)]

    def far(g):
        return [slot(zz, xx) for zz, gg in outer if gg == g for xx in (x, 1 - x)]

    def gate_up(g):
        gi = lax.rem(zp + g, ng)
        at = pl.ds(pl.multiple_of(gi * grows, grows), grows)
        w = wbuf[at, :].astype(jnp.float32)
        lanes = lax.broadcasted_iota(jnp.int32, w.shape, 1)
        outs = []
        dims = (((1,), (1,)), ((), ()))
        for j in range(el):
            col = jnp.sum(jnp.where(lanes == ep * el + j, w, 0.0), axis=1, keepdims=True)
            ga = lax.dot_general(xbuf[at, :], wg[j], dims, preferred_element_type=jnp.float32)
            ua = lax.dot_general(xbuf[at, :], wu[j], dims, preferred_element_type=jnp.float32)
            outs.append((ga / (1.0 + jnp.exp(-ga)) * ua * col).astype(jnp.bfloat16))
        return jnp.concatenate(outs, axis=1)

    def down(g, h):
        for yy in range(2):
            off = pl.ds(pl.multiple_of((yy * 2 + 1 - c) * quarter, LANES), quarter)
            pcs[g, yy] = jnp.dot(h, wd[:, off], preferred_element_type=jnp.float32).astype(jnp.bfloat16)
            go(rc(pcs.at[g, yy], pcr.at[g, yy], rcs.at[g, yy], rcr.at[g, yy], cdev))
        for yy in range(2):
            off = pl.ds(pl.multiple_of((yy * 2 + c) * quarter, LANES), quarter)
            acc[g, yy] = jnp.dot(h, wd[:, off], preferred_element_type=jnp.float32)

    hrows = grows // 2
    xme = pl.ds(pl.multiple_of(x * hrows, hrows), hrows)
    xother = pl.ds(pl.multiple_of((1 - x) * hrows, hrows), hrows)
    k1, k2 = slice(0, part), slice(part, quarter)

    def first(g):
        for yy in range(2):
            rc(pcs.at[g, yy], pcr.at[g, yy], rcs.at[g, yy], rcr.at[g, yy], cdev).wait_recv()
        y1s[g] = (acc[g, 1 - y, :, k1] + pcr[g, 1 - y, :, k1].astype(jnp.float32)).astype(jnp.bfloat16)
        go(rc(y1s.at[g], y1r.at[g], ry1s.at[g], ry1r.at[g], ydev))
        for yy in range(2):
            x2s[g, yy] = (acc[g, yy, xother, k2] + pcr[g, yy, xother, k2].astype(jnp.float32)).astype(jnp.bfloat16)
        go(rc(x2s.at[g], x2r.at[g], rx2s.at[g], rx2r.at[g], xdev))

    def second(g):
        rc(y1s.at[g], y1r.at[g], ry1s.at[g], ry1r.at[g], ydev).wait_recv()

        def kept1(at):
            return (
                acc[g, y, at, k1] + pcr[g, y, at, k1].astype(jnp.float32) + y1r[g, at].astype(jnp.float32)
            )

        x1s[g] = kept1(xother).astype(jnp.bfloat16)
        go(rc(x1s.at[g], x1r.at[g], rx1s.at[g], rx1r.at[g], xdev))
        rc(x2s.at[g], x2r.at[g], rx2s.at[g], rx2r.at[g], xdev).wait_recv()

        def kept2(yy):
            return (
                acc[g, yy, xme, k2] + pcr[g, yy, xme, k2].astype(jnp.float32) + x2r[g, yy].astype(jnp.float32)
            )

        y2s[g] = kept2(1 - y).astype(jnp.bfloat16)
        go(rc(y2s.at[g], y2r.at[g], ry2s.at[g], ry2r.at[g], ydev))
        own[g, :, k1] = kept1(xme)
        own[g, :, k2] = kept2(y)

    def third(g):
        rc(x1s.at[g], x1r.at[g], rx1s.at[g], rx1r.at[g], xdev).wait_recv()
        rc(y2s.at[g], y2r.at[g], ry2s.at[g], ry2r.at[g], ydev).wait_recv()
        own[g, :, k1] += x1r[g].astype(jnp.float32)
        own[g, :, k2] += y2r[g].astype(jnp.float32)
        zs[g] = own[g].astype(jnp.bfloat16)
        for zz in [inner] if g == 0 else [o for o, gg in outer if gg == g]:
            low = pl.ds(pl.multiple_of((zz % 2) * rows, rows), rows)
            go(rc(zs.at[g, low], zr.at[z], rzs.at[zz], rzr.at[z], dev(zz, x, y, c)))

    z_in(inner)
    x_in(z)
    x_in(inner)
    for zz, _ in outer:
        z_in(zz)
    for s_ in near:
        y_in(s_)
    for zz, _ in outer:
        x_in(zz)
    for s_ in near:
        c_in(s_)
    local[5].wait()
    local[6].wait()
    h = gate_up(0)
    local[7].wait()
    down(0, h)
    for g in range(1, ng):
        for s_ in far(g):
            y_in(s_)
    first(0)
    for g in range(1, ng):
        for s_ in far(g):
            c_in(s_)
        h = gate_up(g)
        down(g, h)
        if g == 1:
            second(0)
        first(g)
        if g == 1:
            third(0)
    for g in range(1, ng):
        second(g)
        third(g)
    mylow = pl.ds(pl.multiple_of((z % 2) * rows, rows), rows)
    res = own[0, mylow, :]
    for zz in [inner] + [o for o, _ in outer]:
        rc(zs.at[0, mylow], zr.at[zz], rzs.at[zz], rzr.at[zz], dev(zz, x, y, c)).wait_recv()
        res = res + zr[zz].astype(jnp.float32)
    out[...] = res.astype(jnp.bfloat16)
    for cp in sends:
        cp.wait_send()


def fused(tokens, norm_gain, routes, group_prob, expert_scores, gate_weight, up_weight, down_weight):
    n = lax.axis_size("ep")
    nz = n // 2
    ng = nz // GROUP_Z
    rows, width = tokens.shape
    el, hid, _ = gate_weight.shape
    elanes = -(-el * n // LANES) * LANES
    quarter = width // 4
    part = quarter // 2
    grows = 2 * GROUP_Z * rows
    bf, f32 = jnp.bfloat16, jnp.float32
    dma = pltpu.SemaphoreType.DMA
    anyspec = pl.BlockSpec(memory_space=pl.ANY)
    down2 = down_weight.reshape(el * hid, width)
    return pl.pallas_call(
        functools.partial(kernel, nz),
        out_shape=jax.ShapeDtypeStruct((rows, quarter), bf),
        in_specs=[anyspec] * 8,
        out_specs=pl.BlockSpec(memory_space=pltpu.VMEM),
        scratch_shapes=[
            pltpu.VMEM((rows, width), bf),
            pltpu.VMEM((1, width), f32),
            pltpu.VMEM(routes.shape, routes.dtype),
            pltpu.VMEM((1, rows), f32),
            pltpu.VMEM(expert_scores.shape, f32),
            pltpu.VMEM(gate_weight.shape, bf),
            pltpu.VMEM(up_weight.shape, bf),
            pltpu.VMEM(down2.shape, bf),
            pltpu.VMEM((n * rows, width), bf),
            pltpu.VMEM((n * rows, elanes), bf),
            pltpu.VMEM((ng, 2, grows, quarter), f32),
            pltpu.VMEM((ng, 2, grows, quarter), bf),
            pltpu.VMEM((ng, 2, grows, quarter), bf),
            pltpu.VMEM((ng, grows, part), bf),
            pltpu.VMEM((ng, grows, part), bf),
            pltpu.VMEM((ng, grows // 2, part), bf),
            pltpu.VMEM((ng, grows // 2, part), bf),
            pltpu.VMEM((ng, grows // 2, part), bf),
            pltpu.VMEM((ng, grows // 2, part), bf),
            pltpu.VMEM((ng, 2, grows // 2, part), bf),
            pltpu.VMEM((ng, 2, grows // 2, part), bf),
            pltpu.VMEM((ng, grows // 2, quarter), bf),
            pltpu.VMEM((nz, rows, quarter), bf),
            pltpu.VMEM((ng, grows // 2, quarter), f32),
            dma((8,)),
            *[dma((nz,))] * 8,
            *[dma((n,))] * 4,
            *[dma((ng, 2))] * 2,
            *[dma((ng,))] * 8,
            *[dma((nz,))] * 2,
        ],
        compiler_params=pltpu.CompilerParams(
            collective_id=0, has_side_effects=True, vmem_limit_bytes=60 * 1024 * 1024
        ),
        name="moe_step",
    )(
        tokens, norm_gain.reshape(1, width), routes, group_prob.reshape(1, rows), expert_scores,
        gate_weight, up_weight, down2,
    )


def step(tokens, *rest):
    n = lax.axis_size("ep")
    rows = tokens.shape[0]
    groups = rest[4].shape[0] * n // EXP_GROUP
    cap = min(rows, 2 * (-(-rows // groups)))
    if cap == rows and n % 4 == 0 and n >= 8 and lax.axis_size("tp") == 4 and rows % 16 == 0:
        return fused(tokens, *rest)
    return body(tokens, *rest)


def solution(mesh):
    placed = (
        P("ep", None),
        P(),
        P("ep", None),
        P("ep"),
        P("ep", None),
        P("ep", "tp", None),
        P("ep", "tp", None),
        P("ep", "tp", None),
    )
    return jax.shard_map(step, mesh=mesh, in_specs=placed, out_specs=P("ep", "tp"), check_vma=False)
```

```python
import functools

import jax
import jax.numpy as jnp
from jax import lax
from jax.experimental import pallas as pl
from jax.experimental.pallas import tpu as pltpu
from jax.sharding import PartitionSpec as P

EXP_GROUP = 8


EPS = 1e-06


def body(tokens, norm_gain, routes, group_prob, expert_scores, gate_weight, up_weight, down_weight):
    ep_count = lax.axis_size("ep")
    tp_count = lax.axis_size("tp")
    token_count, model_width = tokens.shape
    expert_local = gate_weight.shape[0]
    expert_total = expert_local * ep_count
    group_total = expert_total // EXP_GROUP
    cap_slots = min(token_count, 2 * ((token_count + group_total - 1) // group_total))
    slot_total = ep_count * cap_slots
    as_float = tokens.astype(jnp.float32)
    normed = (
        as_float
        * lax.rsqrt(jnp.mean(as_float * as_float, axis=-1, keepdims=True) + EPS)
        * norm_gain
    ).astype(jnp.bfloat16)
    mixing = jax.nn.softmax(expert_scores, axis=-1) * group_prob[:, None]
    mixing_half = mixing.astype(jnp.bfloat16)
    dev_of = routes // expert_local
    dev_ids = jnp.arange(ep_count, dtype=jnp.int32)
    touch = jnp.any(dev_of[:, :, None] == dev_ids[None, None, :], axis=1)
    rank = jnp.cumsum(touch.astype(jnp.int32), axis=0) - 1
    slot_td = jnp.where(touch, dev_ids[None, :] * cap_slots + rank, -1)
    slot_range = jnp.arange(slot_total, dtype=jnp.int32)
    matches = jnp.any(slot_td[None, :, :] == slot_range[:, None, None], axis=2)
    onehot = (
        routes[:, :, None] == jnp.arange(expert_total, dtype=jnp.int32)[None, None, :]
    ).astype(jnp.float32)
    weights = jnp.einsum(
        "tke,tk->te", onehot, mixing_half.astype(jnp.float32), precision=lax.Precision.HIGHEST
    ).reshape(token_count, ep_count, expert_local)
    out_weights = jnp.einsum(
        "dct,tdj->dcj",
        matches.reshape(ep_count, cap_slots, token_count).astype(jnp.float32),
        weights,
        precision=lax.Precision.HIGHEST,
    ).astype(jnp.bfloat16)
    share = model_width // tp_count
    payload = lax.dynamic_slice_in_dim(normed, lax.axis_index("tp") * share, share, 1)
    outgoing = jnp.dot(
        matches.astype(jnp.bfloat16), payload, preferred_element_type=jnp.float32
    ).astype(jnp.bfloat16)
    outgoing = outgoing.reshape(ep_count, cap_slots, payload.shape[1])
    rows = lax.all_to_all(outgoing, "ep", split_axis=0, concat_axis=0, tiled=True)
    row_weights = lax.all_to_all(out_weights, "ep", split_axis=0, concat_axis=0, tiled=True)
    rows = lax.all_gather(rows, "tp", axis=2, tiled=True)
    gate_act = jnp.einsum("scd,jfd->scjf", rows, gate_weight, preferred_element_type=jnp.float32)
    up_act = jnp.einsum("scd,jfd->scjf", rows, up_weight, preferred_element_type=jnp.float32)
    hidden = (
        jax.nn.silu(gate_act) * up_act * row_weights.astype(jnp.float32)[:, :, :, None]
    ).astype(jnp.bfloat16)
    partial_value = jnp.einsum(
        "scjf,jfd->scd", hidden, down_weight, preferred_element_type=jnp.float32
    ).astype(jnp.bfloat16)
    summed = lax.psum_scatter(partial_value, "tp", scatter_dimension=2, tiled=True).astype(
        jnp.float32
    )
    returned = lax.all_to_all(
        summed.astype(jnp.bfloat16), "ep", split_axis=0, concat_axis=0, tiled=True
    )
    gathered_rows = returned.reshape(slot_total, returned.shape[2]).astype(jnp.float32)
    result = jnp.dot(matches.T.astype(jnp.float32), gathered_rows, precision=lax.Precision.HIGHEST)
    return result.astype(jnp.bfloat16)


GROUP_Z = 2
LANES = 128
MESH = pl.DeviceIdType.MESH


def kernel(
    nz, tokens, gain, routes, prob, scores, gate_hbm, up_hbm, down_hbm, out,
    tok, gain_v, routes_v, prob_v, scores_v, wg, wu, wd, xbuf, wbuf, acc, pcs, pcr,
    y1s, y1r, x1s, x1r, y2s, y2r, x2s, x2r, zs, zr, own,
    loc, azs, azr, wzs, wzr, axs, axr, wxs, wxr, ays, ayr, acs, acr,
    rcs, rcr, ry1s, ry1r, rx1s, rx1r, ry2s, ry2r, rx2s, rx2r, rzs, rzr,
):
    ep, tp = lax.axis_index("ep"), lax.axis_index("tp")
    z, x = ep // 2, ep % 2
    y, c = tp // 2, tp % 2
    rows, width = tokens.shape
    el, hid, _ = gate_hbm.shape
    ng = nz // GROUP_Z
    grows = 2 * GROUP_Z * rows
    half = width // 2
    quarter = width // 4
    part = quarter // 2
    gcols = half // 2

    def dev(z_, x_, y_, c_):
        return (z_ * 2 + x_, y_ * 2 + c_)

    xdev, ydev, cdev = dev(z, 1 - x, y, c), dev(z, x, 1 - y, c), dev(z, x, y, 1 - c)
    zof = [lax.rem(z + d, nz) for d in range(nz)]

    def rc(src, dst, ss, rs, to):
        return pltpu.make_async_remote_copy(
            src_ref=src, dst_ref=dst, send_sem=ss, recv_sem=rs, device_id=to, device_id_type=MESH
        )

    pairs = [
        (tokens, tok), (gain, gain_v), (routes, routes_v), (prob, prob_v), (scores, scores_v),
        (gate_hbm, wg), (up_hbm, wu), (down_hbm, wd),
    ]
    local = [pltpu.make_async_copy(s, d, loc.at[i]) for i, (s, d) in enumerate(pairs)]
    for cp in local:
        cp.start()
    barrier = pltpu.get_barrier_semaphore()
    friends = [xdev, ydev, cdev] + [dev(zz, x, y, c) for zz in zof[1:]]
    for to in friends:
        pl.semaphore_signal(barrier, inc=1, device_id=to, device_id_type=MESH)

    def slot(z_, x_):
        return ((z_ // 2) * 2 + x_) * 2 + z_ % 2

    def rowsof(s):
        return pl.ds(pl.multiple_of(s * rows, rows), rows)

    for cp in local[:5]:
        cp.wait()
    mine = slot(z, x)
    step = 16
    wide = 4 * LANES
    for r in range(0, rows, step):
        total = jnp.zeros((step, wide), jnp.float32)
        for k in range(0, width, wide):
            v = tok[r : r + step, k : k + wide].astype(jnp.float32)
            total += v * v
        scale = lax.rsqrt(jnp.sum(total, axis=1, keepdims=True) / width + EPS)
        at = pl.ds(pl.multiple_of(mine * rows + r, step), step)
        for k in range(0, width, wide):
            v = tok[r : r + step, k : k + wide].astype(jnp.float32)
            xbuf[at, k : k + wide] = (v * scale * gain_v[:, k : k + wide]).astype(jnp.bfloat16)
    diag = lax.broadcasted_iota(jnp.int32, (rows, rows), 0) == lax.broadcasted_iota(
        jnp.int32, (rows, rows), 1
    )

    def column(row):
        return jnp.sum(jnp.where(diag, jnp.broadcast_to(row, (rows, rows)), 0.0), axis=1, keepdims=True)

    e = jnp.exp(scores_v[...] - jnp.max(scores_v[...], axis=0, keepdims=True))
    mix = (e / jnp.sum(e, axis=0, keepdims=True) * prob_v[...]).astype(jnp.bfloat16).astype(jnp.float32)
    lane = lax.broadcasted_iota(jnp.int32, (rows, wbuf.shape[1]), 1).astype(jnp.float32)
    wm = jnp.zeros((rows, wbuf.shape[1]), jnp.float32)
    rt = routes_v[...].astype(jnp.float32)
    for k in range(rt.shape[0]):
        wm += jnp.where(column(rt[k : k + 1, :]) == lane, column(mix[k : k + 1, :]), 0.0)
    wbuf[rowsof(mine), :] = wm.astype(jnp.bfloat16)

    pl.semaphore_wait(barrier, len(friends))

    def cols(c_, y_):
        return pl.ds(pl.multiple_of(c_ * half + y_ * gcols, LANES), gcols)

    gc = cols(c, y)

    sends = []

    def go(cp):
        cp.start()
        sends.append(cp)

    def x_out(zz):
        b = rowsof(slot(zz, x))
        go(rc(xbuf.at[b, gc], xbuf.at[b, gc], axs.at[zz], axr.at[zz], xdev))
        go(rc(wbuf.at[b], wbuf.at[b], wxs.at[zz], wxr.at[zz], xdev))

    def plane_out(s_):
        b = rowsof(s_)
        go(rc(xbuf.at[b, gc], xbuf.at[b, gc], ays.at[s_], ayr.at[s_], ydev))
        go(rc(xbuf.at[b, gc], xbuf.at[b, gc], acs.at[s_, y], acr.at[s_, y], cdev))

    b = rowsof(mine)
    x_out(z)

    zp = z // 2
    inner = zp * 2 + 1 - z % 2
    outer = [(lax.rem(zp + g, ng) * 2 + low, g) for g in range(1, ng) for low in range(2)]
    for zz in [inner] + [o for o, _ in outer]:
        go(rc(xbuf.at[b, gc], xbuf.at[b, gc], azs.at[zz], azr.at[z], dev(zz, x, y, c)))
        go(rc(wbuf.at[b], wbuf.at[b], wzs.at[zz], wzr.at[z], dev(zz, x, y, c)))

    def z_in(zz):
        r_ = rowsof(slot(zz, x))
        to = dev(zz, x, y, c)
        rc(xbuf.at[r_, gc], xbuf.at[r_, gc], azs.at[zz], azr.at[zz], to).wait_recv()
        rc(wbuf.at[r_], wbuf.at[r_], wzs.at[zz], wzr.at[zz], to).wait_recv()
        x_out(zz)
        plane_out(slot(zz, x))

    def x_in(zz):
        r_ = rowsof(slot(zz, 1 - x))
        rc(xbuf.at[r_, gc], xbuf.at[r_, gc], axs.at[zz], axr.at[zz], xdev).wait_recv()
        rc(wbuf.at[r_], wbuf.at[r_], wxs.at[zz], wxr.at[zz], xdev).wait_recv()
        plane_out(slot(zz, 1 - x))

    def y_in(s_):
        r_, cc = rowsof(s_), cols(c, 1 - y)
        rc(xbuf.at[r_, cc], xbuf.at[r_, cc], ays.at[s_], ayr.at[s_], ydev).wait_recv()
        go(rc(xbuf.at[r_, cc], xbuf.at[r_, cc], acs.at[s_, 1 - y], acr.at[s_, 1 - y], cdev))

    def c_in(s_):
        r_ = rowsof(s_)
        for y_ in range(2):
            cc = cols(1 - c, y_)
            rc(xbuf.at[r_, cc], xbuf.at[r_, cc], acs.at[s_, y_], acr.at[s_, y_], cdev).wait_recv()

    near = [slot(inner, x), slot(z, 1 - x), slot(inner, 1 - x)]

    def far(g):
        return [slot(zz, xx) for zz, gg in outer if gg == g for xx in (x, 1 - x)]

    def gate_up(g):
        gi = lax.rem(zp + g, ng)
        at = pl.ds(pl.multiple_of(gi * grows, grows), grows)
        w = wbuf[at, :].astype(jnp.float32)
        lanes = lax.broadcasted_iota(jnp.int32, w.shape, 1)
        outs = []
        dims = (((1,), (1,)), ((), ()))
        for j in range(el):
            col = jnp.sum(jnp.where(lanes == ep * el + j, w, 0.0), axis=1, keepdims=True)
            ga = lax.dot_general(xbuf[at, :], wg[j], dims, preferred_element_type=jnp.float32)
            ua = lax.dot_general(xbuf[at, :], wu[j], dims, preferred_element_type=jnp.float32)
            outs.append((ga / (1.0 + jnp.exp(-ga)) * ua * col).astype(jnp.bfloat16))
        return jnp.concatenate(outs, axis=1)

    def down(g, h):
        for yy in range(2):
            off = pl.ds(pl.multiple_of((yy * 2 + 1 - c) * quarter, LANES), quarter)
            pcs[g, yy] = jnp.dot(h, wd[:, off], preferred_element_type=jnp.float32).astype(jnp.bfloat16)
            go(rc(pcs.at[g, yy], pcr.at[g, yy], rcs.at[g, yy], rcr.at[g, yy], cdev))
        for yy in range(2):
            off = pl.ds(pl.multiple_of((yy * 2 + c) * quarter, LANES), quarter)
            acc[g, yy] = jnp.dot(h, wd[:, off], preferred_element_type=jnp.float32)

    hrows = grows // 2
    xme = pl.ds(pl.multiple_of(x * hrows, hrows), hrows)
    xother = pl.ds(pl.multiple_of((1 - x) * hrows, hrows), hrows)
    k1, k2 = slice(0, part), slice(part, quarter)

    def first(g):
        for yy in range(2):
            rc(pcs.at[g, yy], pcr.at[g, yy], rcs.at[g, yy], rcr.at[g, yy], cdev).wait_recv()
        y1s[g] = (acc[g, 1 - y, :, k1] + pcr[g, 1 - y, :, k1].astype(jnp.float32)).astype(jnp.bfloat16)
        go(rc(y1s.at[g], y1r.at[g], ry1s.at[g], ry1r.at[g], ydev))
        for yy in range(2):
            x2s[g, yy] = (acc[g, yy, xother, k2] + pcr[g, yy, xother, k2].astype(jnp.float32)).astype(jnp.bfloat16)
        go(rc(x2s.at[g], x2r.at[g], rx2s.at[g], rx2r.at[g], xdev))

    def second(g):
        rc(y1s.at[g], y1r.at[g], ry1s.at[g], ry1r.at[g], ydev).wait_recv()

        def kept1(at):
            return (
                acc[g, y, at, k1] + pcr[g, y, at, k1].astype(jnp.float32) + y1r[g, at].astype(jnp.float32)
            )

        x1s[g] = kept1(xother).astype(jnp.bfloat16)
        go(rc(x1s.at[g], x1r.at[g], rx1s.at[g], rx1r.at[g], xdev))
        rc(x2s.at[g], x2r.at[g], rx2s.at[g], rx2r.at[g], xdev).wait_recv()

        def kept2(yy):
            return (
                acc[g, yy, xme, k2] + pcr[g, yy, xme, k2].astype(jnp.float32) + x2r[g, yy].astype(jnp.float32)
            )

        y2s[g] = kept2(1 - y).astype(jnp.bfloat16)
        go(rc(y2s.at[g], y2r.at[g], ry2s.at[g], ry2r.at[g], ydev))
        own[g, :, k1] = kept1(xme)
        own[g, :, k2] = kept2(y)

    def third(g):
        rc(x1s.at[g], x1r.at[g], rx1s.at[g], rx1r.at[g], xdev).wait_recv()
        rc(y2s.at[g], y2r.at[g], ry2s.at[g], ry2r.at[g], ydev).wait_recv()
        own[g, :, k1] += x1r[g].astype(jnp.float32)
        own[g, :, k2] += y2r[g].astype(jnp.float32)
        zs[g] = own[g].astype(jnp.bfloat16)
        for zz in [inner] if g == 0 else [o for o, gg in outer if gg == g]:
            low = pl.ds(pl.multiple_of((zz % 2) * rows, rows), rows)
            go(rc(zs.at[g, low], zr.at[z], rzs.at[zz], rzr.at[z], dev(zz, x, y, c)))

    z_in(inner)
    x_in(z)
    x_in(inner)
    for zz, _ in outer:
        z_in(zz)
    for s_ in near:
        y_in(s_)
    for zz, _ in outer:
        x_in(zz)
    for s_ in near:
        c_in(s_)
    local[5].wait()
    local[6].wait()
    h = gate_up(0)
    local[7].wait()
    down(0, h)
    for g in range(1, ng):
        for s_ in far(g):
            y_in(s_)
    first(0)
    for g in range(1, ng):
        for s_ in far(g):
            c_in(s_)
        h = gate_up(g)
        down(g, h)
        if g == 1:
            second(0)
        first(g)
        if g == 1:
            third(0)
    for g in range(1, ng):
        second(g)
        third(g)
    mylow = pl.ds(pl.multiple_of((z % 2) * rows, rows), rows)
    res = own[0, mylow, :]
    for zz in [inner] + [o for o, _ in outer]:
        rc(zs.at[0, mylow], zr.at[zz], rzs.at[zz], rzr.at[zz], dev(zz, x, y, c)).wait_recv()
        res = res + zr[zz].astype(jnp.float32)
    out[...] = res.astype(jnp.bfloat16)
    for cp in sends:
        cp.wait_send()


def fused(tokens, norm_gain, routes, group_prob, expert_scores, gate_weight, up_weight, down_weight):
    n = lax.axis_size("ep")
    nz = n // 2
    ng = nz // GROUP_Z
    rows, width = tokens.shape
    el, hid, _ = gate_weight.shape
    elanes = -(-el * n // LANES) * LANES
    quarter = width // 4
    part = quarter // 2
    grows = 2 * GROUP_Z * rows
    bf, f32 = jnp.bfloat16, jnp.float32
    dma = pltpu.SemaphoreType.DMA
    anyspec = pl.BlockSpec(memory_space=pl.ANY)
    down2 = down_weight.reshape(el * hid, width)
    return pl.pallas_call(
        functools.partial(kernel, nz),
        out_shape=jax.ShapeDtypeStruct((rows, quarter), bf),
        in_specs=[anyspec] * 8,
        out_specs=pl.BlockSpec(memory_space=pltpu.VMEM),
        scratch_shapes=[
            pltpu.VMEM((rows, width), bf),
            pltpu.VMEM((1, width), f32),
            pltpu.VMEM(routes.shape[::-1], routes.dtype),
            pltpu.VMEM((1, rows), f32),
            pltpu.VMEM(expert_scores.shape[::-1], f32),
            pltpu.VMEM(gate_weight.shape, bf),
            pltpu.VMEM(up_weight.shape, bf),
            pltpu.VMEM(down2.shape, bf),
            pltpu.VMEM((n * rows, width), bf),
            pltpu.VMEM((n * rows, elanes), bf),
            pltpu.VMEM((ng, 2, grows, quarter), f32),
            pltpu.VMEM((ng, 2, grows, quarter), bf),
            pltpu.VMEM((ng, 2, grows, quarter), bf),
            pltpu.VMEM((ng, grows, part), bf),
            pltpu.VMEM((ng, grows, part), bf),
            pltpu.VMEM((ng, grows // 2, part), bf),
            pltpu.VMEM((ng, grows // 2, part), bf),
            pltpu.VMEM((ng, grows // 2, part), bf),
            pltpu.VMEM((ng, grows // 2, part), bf),
            pltpu.VMEM((ng, 2, grows // 2, part), bf),
            pltpu.VMEM((ng, 2, grows // 2, part), bf),
            pltpu.VMEM((ng, grows // 2, quarter), bf),
            pltpu.VMEM((nz, rows, quarter), bf),
            pltpu.VMEM((ng, grows // 2, quarter), f32),
            dma((8,)),
            *[dma((nz,))] * 8,
            *[dma((n,))] * 2,
            *[dma((n, 2))] * 2,
            *[dma((ng, 2))] * 2,
            *[dma((ng,))] * 8,
            *[dma((nz,))] * 2,
        ],
        compiler_params=pltpu.CompilerParams(
            collective_id=0, has_side_effects=True, vmem_limit_bytes=60 * 1024 * 1024
        ),
        name="moe_step",
    )(
        tokens, norm_gain.reshape(1, width), routes.T, group_prob.reshape(1, rows), expert_scores.T,
        gate_weight, up_weight, down2,
    )


def step(tokens, *rest):
    n = lax.axis_size("ep")
    rows = tokens.shape[0]
    groups = rest[4].shape[0] * n // EXP_GROUP
    cap = min(rows, 2 * (-(-rows // groups)))
    if cap == rows and n % 4 == 0 and n >= 8 and lax.axis_size("tp") == 4 and rows % 16 == 0:
        return fused(tokens, *rest)
    return body(tokens, *rest)


def solution(mesh):
    placed = (
        P("ep", None),
        P(),
        P("ep", None),
        P("ep"),
        P("ep", None),
        P("ep", "tp", None),
        P("ep", "tp", None),
        P("ep", "tp", None),
    )
    return jax.shard_map(step, mesh=mesh, in_specs=placed, out_specs=P("ep", "tp"), check_vma=False)
```
